32 devices in a mesh: row: 4 (over y, x), col: 8 (over z, core).
Axes of the slice: x: 2, y: 2, z: 4, core: 2. Of those that a mesh axis runs over, the one named last changes fastest.
Arguments:
- mix_input: bfloat16 [4, 4096, 512], P(None, ('row', 'col')), may hold values from -6 to 6
- group_maps: bfloat16 [4, 128, 128], replicated, may hold values from -0.5 to 0.5
- out_map: bfloat16 [512, 2048], replicated, may hold values from -0.25 to 0.25
Outputs:
- mixed: bfloat16 [4, 4096, 2048], P(None, ('row', 'col'))
The draws below stay inside these ranges and needn't reach their ends.
All inputs are finite; a program needn't handle non-finite values.
Results may differ from the reference program's by a relative error of at most 0.011.
Values may be sent and summed in bfloat16 or wider, within the bound.
A program may use at most 64 MiB of HBM per device.

```python
import jax
import jax.numpy as jnp
from jax import lax

MODEL = 2048
GROUPS = 4
GROUP_CH = 128
SEQS = 4
CHANNELS = 512
LENGTH = 4096


def level_of(stream_key, shape, cuts, low, high):
    gain, own = 1.0, jax.random.fold_in(stream_key, 6)
    for axis_at, parts in cuts:
        heights = jnp.exp(jax.random.uniform(jax.random.fold_in(own, axis_at), (parts,), jnp.float32, low / len(cuts), high / len(cuts)))
        gain = gain * jnp.repeat(heights, shape[axis_at] // parts).reshape([-1 if axis == axis_at else 1 for axis in range(len(shape))])
    return gain


def centred(stream_key, dims, width, reach, shards=(), held_as=jnp.bfloat16):
    values = jax.random.normal(stream_key, dims, jnp.float32) * width
    if len(shards) > 0:
        values = level_of(stream_key, dims, shards, -0.22, 0.18) * values
    return jnp.clip(values, min=-reach, max=reach).astype(held_as)


def setup_inputs(seed: int = 0) -> dict:
    key_of = jax.random.split(jax.random.key(seed), 4)
    return {
        "mix_input": centred(key_of[0], (SEQS, LENGTH, CHANNELS), 1.0, 6.0, ((1, 32),)),
        "group_maps": centred(key_of[1], (GROUPS, GROUP_CH, GROUP_CH), GROUP_CH ** -0.5, 0.5),
        "out_map": centred(key_of[2], (CHANNELS, MODEL), CHANNELS ** -0.5, 0.25),
    }


def reference(mix_input, group_maps, out_map):
    def one_sequence(sequence):
        signal = sequence.astype(jnp.float32).reshape(LENGTH, GROUPS, GROUP_CH)
        spectrum = jnp.fft.fft2(signal, axes=(0, 2), norm="ortho").real.astype(jnp.float32)
        spectrum = spectrum.astype(jnp.bfloat16)
        grouped = jnp.einsum("pgj,gjl->pgl", spectrum.astype(jnp.float32), group_maps.astype(jnp.float32))
        grouped = grouped.astype(jnp.bfloat16).reshape(LENGTH, CHANNELS)
        return jnp.dot(grouped, out_map, preferred_element_type=jnp.float32).astype(jnp.bfloat16)

    return lax.map(one_sequence, mix_input)
```

```python
import math

import jax
import jax.numpy as jnp
import numpy as np
from jax import lax
from jax.experimental import pallas as pl
from jax.experimental.pallas import tpu as pltpu
from jax.sharding import PartitionSpec as P

AXES = ("row", "col")


def turn_tables(left_count, right_count, modulus):
    turns = np.arange(left_count)[:, None] * np.arange(right_count)[None, :] % modulus
    angles = turns * (2.0 * math.pi / modulus)
    return np.cos(angles), np.sin(angles)


def lane_tables(width):
    cosine, sine = turn_tables(width, width, width)
    half = width // 2
    pack = np.zeros((width, width))
    unpack = np.zeros((width, width))
    pack[:, 0::2] = cosine[:, :half]
    pack[:, 1::2] = -sine[:, :half]
    pack[:, 1] = cosine[:, half]
    unpack[0, 0] = 1.0
    unpack[1, half] = 1.0
    for freq in range(1, half):
        unpack[2 * freq, freq] = unpack[2 * freq, width - freq] = 1.0
        unpack[2 * freq + 1, freq] = 1.0
        unpack[2 * freq + 1, width - freq] = -1.0
    return pack, unpack


def fourier(values):
    count = len(values)
    if count == 1:
        return values
    even, odd = fourier(values[0::2]), fourier(values[1::2])
    low, high = [], []
    for at in range(count // 2):
        cosine = math.cos(2.0 * math.pi * at / count)
        sine = math.sin(2.0 * math.pi * at / count)
        (even_re, even_im), (odd_re, odd_im) = even[at], odd[at]
        if at == 0:
            turn_re, turn_im = odd_re, odd_im
        elif 4 * at == count:
            turn_re, turn_im = odd_im, -odd_re
        elif odd_im is None:
            turn_re, turn_im = odd_re * cosine, odd_re * -sine
        else:
            turn_re = odd_re * cosine + odd_im * sine
            turn_im = odd_im * cosine - odd_re * sine
        if turn_re is None:
            low_re = high_re = even_re
        else:
            low_re, high_re = even_re + turn_re, even_re - turn_re
        if turn_im is None:
            low_im = high_im = even_im
        elif even_im is None:
            low_im, high_im = turn_im, -turn_im
        else:
            low_im, high_im = even_im + turn_im, even_im - turn_im
        low.append((low_re, low_im))
        high.append((high_re, high_im))
    return low + high


def mixing_kernel(
    x_hbm, pack_hbm, cos_hbm, sin_hbm, table_hbm, unpack_hbm, given_hbm, outs_hbm, out_ref,
    x_ref, pack_ref, cos_ref, sin_ref, table_ref, unpack_ref, given_ref, outs_ref, weights, load_sem,
    send, held, stack, big, send_back, back, near, send_sem, recv_sem, send_back_sem, recv_back_sem,
):
    bf16, f32 = jnp.bfloat16, jnp.float32
    seqs, positions, channels = x_ref.shape
    devices, items, _ = send.shape
    width = pack_ref.shape[0]
    groups = channels // width
    cols = lax.axis_size("col")
    row, col = lax.axis_index("row"), lax.axis_index("col")
    me = row * cols + col
    mesh_ids = pl.DeviceIdType.MESH
    my_x, my_y = lax.rem(row, 2), lax.div(row, 2)
    my_core, my_low, my_high = lax.rem(col, 2), lax.rem(lax.div(col, 2), 2), lax.div(col, 4)
    members = devices // seqs
    my_seq = 2 * my_core + lax.rem(my_x + my_y + my_low, 2)
    my_slot = my_seq * members + row * 2 + my_high

    far_refs = (pack_hbm, unpack_hbm, given_hbm, outs_hbm, cos_hbm, sin_hbm, table_hbm)
    near_refs = (pack_ref, unpack_ref, given_ref, outs_ref, cos_ref, sin_ref, table_ref)
    x_loads = [
        pltpu.make_async_copy(x_hbm.at[s], x_ref.at[s], load_sem.at[s]) for s in range(seqs)
    ]
    loads = [
        pltpu.make_async_copy(src, dst, load_sem.at[seqs + at])
        for at, (src, dst) in enumerate(zip(far_refs, near_refs))
    ]
    x_loads[0].start()
    for load in (loads[0], *x_loads[1:], *loads[1:]):
        load.start()
    barrier = pltpu.get_barrier_semaphore()

    def turned(step):
        x = lax.rem(my_x + lax.rem(step, 2), 2)
        y = lax.rem(my_y + lax.rem(lax.div(step, 2), 2), 2)
        core = lax.rem(my_core + lax.rem(lax.div(step, 4), 2), 2)
        low = lax.rem(my_low + lax.rem(lax.div(step, 8), 2), 2)
        high = lax.rem(my_high + lax.div(step, 16), 2)
        return y * 2 + x, high * 4 + low * 2 + core

    def greet(step, carry):
        pl.semaphore_signal(
            barrier, inc=1, device_id=turned(devices - step), device_id_type=mesh_ids
        )
        return carry

    lax.fori_loop(1, devices, greet, 0)
    rows_t = (((1,), (1,)), ((), ()))

    def slot_copy(src, src_at, dst, dst_at, out_sem, in_sem, where):
        return pltpu.make_async_remote_copy(
            src_ref=src.at[src_at], dst_ref=dst.at[dst_at], send_sem=out_sem, recv_sem=in_sem,
            device_id=where, device_id_type=mesh_ids,
        )

    def several(src, dst, count, out_sem, in_sem):
        return slot_copy(src, pl.ds(0, count), dst, pl.ds(0, count), out_sem, in_sem, (row, col))

    for s in range(seqs):
        x_loads[s].wait()
        if s == 0:
            loads[0].wait()
        for g in range(groups):
            lanes = lax.dot_general(
                pack_ref[...], x_ref[s, :, g * width : (g + 1) * width], rows_t,
                preferred_element_type=f32,
            ).astype(bf16)
            for half in range(2):
                send[(s * groups + g) * 2 + half] = lanes[half * items : (half + 1) * items]
        if s == 0:
            pl.semaphore_wait(barrier, devices - 1)

        def start(step, carry):
            x = lax.rem(my_x + lax.rem(step, 2), 2)
            y = lax.rem(my_y + lax.rem(lax.div(step, 2), 2), 2)
            high = lax.rem(my_high + lax.div(step, 4), 2)
            low = lax.rem(s % 2 + x + y, 2)
            to_row, to_col = y * 2 + x, high * 4 + low * 2 + s // 2
            slot_copy(
                send, s * members + to_row * 2 + high, held, me, send_sem, recv_sem, (to_row, to_col)
            ).start()
            return carry

        lax.fori_loop(jnp.where(my_seq == s, 1, 0), members, start, 0)
    held[me] = send[my_slot]

    for load in loads[1:4]:
        load.wait()
    for g in range(groups):
        rows = slice(g * width, (g + 1) * width)
        maps = jnp.dot(unpack_ref[...], given_ref[g], preferred_element_type=f32).astype(bf16)
        weights[rows, :] = jnp.dot(
            maps, outs_ref[rows, :], preferred_element_type=f32
        ).astype(bf16)
    for load in loads[4:]:
        load.wait()
    several(send, held, devices - 1, send_sem, recv_sem).wait_recv()

    tile = 16
    def spin(chunk, carry):
        rows = pl.ds(pl.multiple_of(chunk * tile, tile), tile)
        spun = fourier([(held[d, rows, :].astype(f32), None) for d in range(devices)])
        row_ids = chunk * tile + lax.broadcasted_iota(jnp.int32, (tile, positions), 0)
        lane_ids = lax.rem(my_slot * items + row_ids, width)
        is_sine = (lax.rem(lane_ids, 2) == 1) & (lane_ids != 1)
        for f in range(devices):
            real_in, imag_in = spun[f]
            cosine, sine = cos_ref[f : f + 1, :], sin_ref[f : f + 1, :]
            if imag_in is None:
                real_part, imag_part = real_in * cosine, -(real_in * sine)
            else:
                real_part = real_in * cosine + imag_in * sine
                imag_part = imag_in * cosine - real_in * sine
            stack[f, rows, :positions] = jnp.where(is_sine, -imag_part, real_part).astype(bf16)
            stack[f, rows, positions:] = jnp.where(is_sine, real_part, imag_part).astype(bf16)
        return carry

    lax.fori_loop(0, items // tile, spin, 0)
    pairs = devices // 2
    for a in range(pairs):
        both = jnp.concatenate([stack[a], stack[a + pairs]], axis=0)
        big[pl.ds(a, positions, stride=pairs), :] = lax.dot_general(
            table_ref[...], both, rows_t, preferred_element_type=f32
        )
    for e in range(devices):
        send_back[e] = big[e * items : (e + 1) * items, :].astype(bf16)

    def start_back(step, carry):
        to_row, to_col = turned(step)
        slot_copy(
            send_back, to_row * cols + to_col, back, my_slot, send_back_sem,
            recv_back_sem.at[my_seq], (to_row, to_col),
        ).start()
        return carry

    lax.fori_loop(1, devices, start_back, 0)
    back[my_slot] = send_back[me]
    several(send, held, devices - 1, send_sem, recv_sem).wait_send()

    left = lax.broadcasted_iota(jnp.int32, (items, width), 1) < items
    chunk = 512

    def finish(s, carry):
        @pl.when(my_seq == s)
        def _():
            several(send_back, back, members - 1, send_back_sem, recv_back_sem.at[s]).wait_recv()

        @pl.when(my_seq != s)
        def _():
            several(send_back, back, members, send_back_sem, recv_back_sem.at[s]).wait_recv()

        for g in range(groups):
            slot = s * members + g * 2
            first, second = back[slot].astype(f32), back[slot + 1].astype(f32)
            lanes = slice(g * width, (g + 1) * width)
            near[:items, lanes] = jnp.where(left, first, pltpu.roll(second, items, 1)).astype(bf16)
            near[items:, lanes] = jnp.where(left, pltpu.roll(first, items, 1), second).astype(bf16)
        for at in range(0, weights.shape[1], chunk):
            made = jnp.dot(
                near[...], weights[:, at : at + chunk], preferred_element_type=f32
            ).astype(bf16)
            for h in range(2):
                for m in range(items // pairs):
                    base, had = m * devices + h * pairs, h * items + m * pairs
                    out_ref[s, base : base + pairs, at : at + chunk] = made[had : had + pairs]
        return carry

    lax.fori_loop(0, seqs, finish, 0)
    several(send_back, back, devices - 1, send_back_sem, recv_back_sem.at[0]).wait_send()


def fused_lanes(mix_input, group_maps, out_map, pack, unpack, devices, scale):
    bf16, f32 = jnp.bfloat16, jnp.float32
    seqs, positions, channels = mix_input.shape
    width = pack.shape[0]
    items = seqs * channels // devices
    length = devices * positions
    twist_cos, twist_sin = turn_tables(devices, positions, length)
    pos_cos, pos_sin = turn_tables(positions, positions, positions)
    table = np.concatenate([pos_cos, pos_sin], axis=1) * scale
    slots = (devices, items, positions)
    hbm = pl.BlockSpec(memory_space=pltpu.HBM)
    dma = pltpu.SemaphoreType.DMA
    return pl.pallas_call(
        mixing_kernel,
        out_shape=pltpu.VMEM((seqs, positions, out_map.shape[1]), bf16),
        in_specs=[hbm] * 8,
        out_specs=pl.BlockSpec(memory_space=pltpu.VMEM),
        scratch_shapes=[
            pltpu.VMEM(mix_input.shape, bf16), pltpu.VMEM(pack.shape, bf16),
            pltpu.VMEM(twist_cos.shape, f32), pltpu.VMEM(twist_sin.shape, f32),
            pltpu.VMEM(table.shape, bf16), pltpu.VMEM(unpack.shape, bf16),
            pltpu.VMEM(group_maps.shape, bf16), pltpu.VMEM(out_map.shape, bf16),
            pltpu.VMEM(out_map.shape, bf16), dma((seqs + 7,)),
            pltpu.VMEM(slots, bf16), pltpu.VMEM(slots, bf16),
            pltpu.VMEM((devices, items, 2 * positions), bf16),
            pltpu.VMEM((devices * items, width), f32),
            pltpu.VMEM(slots, bf16), pltpu.VMEM(slots, bf16),
            pltpu.VMEM((2 * items, channels), bf16),
            dma, dma, dma, dma((seqs,)),
        ],
        compiler_params=pltpu.CompilerParams(
            collective_id=0, has_side_effects=True
        ),
    )(
        mix_input, jnp.asarray(pack.T, bf16), jnp.asarray(twist_cos, f32),
        jnp.asarray(twist_sin, f32), jnp.asarray(table, bf16), jnp.asarray(unpack, bf16), group_maps,
        out_map,
    )


def exchanged_lanes(mix_input, pack, width, devices, me, scale):
    bf16, f32 = jnp.bfloat16, jnp.float32
    seqs, positions, channels = mix_input.shape
    groups = channels // width
    length = devices * positions
    items = seqs * channels // devices
    lanes = jnp.einsum(
        "spgj,jc->sgcp",
        mix_input.reshape(seqs, positions, groups, width),
        jnp.asarray(pack, bf16),
        preferred_element_type=f32,
    ).astype(bf16)
    sent = lanes.reshape(devices, items, positions)
    held = lax.all_to_all(sent, AXES, split_axis=0, concat_axis=0, tiled=True)

    dev_cos, dev_sin = turn_tables(devices, devices, devices)
    both = jnp.asarray(np.concatenate([dev_cos, -dev_sin], axis=1), bf16)
    spun = jnp.einsum("df,dnp->fnp", both, held, preferred_element_type=f32)
    real_in, imag_in = spun[:devices], spun[devices:]
    twist_cos, twist_sin = turn_tables(devices, positions, length)
    twist_cos = jnp.asarray(twist_cos, f32)[:, None, :]
    twist_sin = jnp.asarray(twist_sin, f32)[:, None, :]
    real_part = real_in * twist_cos + imag_in * twist_sin
    imag_part = imag_in * twist_cos - real_in * twist_sin
    lane_ids = (me * items + jnp.arange(items, dtype=jnp.int32)) % width
    is_sine = ((lane_ids % 2 == 1) & (lane_ids != 1))[None, :, None]
    first = jnp.where(is_sine, -imag_part, real_part).astype(bf16)
    second = jnp.where(is_sine, real_part, imag_part).astype(bf16)
    stacked = jnp.concatenate([first, second], axis=2)
    pos_cos, pos_sin = turn_tables(positions, positions, positions)
    pos_table = jnp.asarray(np.concatenate([pos_cos, pos_sin], axis=0) * scale, bf16)
    freqs = jnp.einsum("pm,fnp->mfn", pos_table, stacked, preferred_element_type=f32).astype(bf16)

    freqs = freqs.reshape(devices, positions, items)
    back = lax.all_to_all(freqs, AXES, split_axis=0, concat_axis=0, tiled=True)
    parts = width // items
    back = back.reshape(seqs, groups, parts, positions, items)
    return back.transpose(0, 3, 1, 2, 4).reshape(seqs * positions, groups, width)


def per_device(mix_input, group_maps, out_map):
    bf16, f32 = jnp.bfloat16, jnp.float32
    seqs, positions, channels = mix_input.shape
    groups, width, _ = group_maps.shape
    devices = lax.axis_size("row") * lax.axis_size("col")
    me = lax.axis_index("row") * lax.axis_size("col") + lax.axis_index("col")
    items = seqs * channels // devices
    pack, unpack = lane_tables(width)
    scale = 1.0 / math.sqrt(devices * positions * width)
    square = 2 * items == width and positions == width and items == 2 * devices
    if square and lax.axis_size("col") == 8 and seqs == 4:
        return fused_lanes(mix_input, group_maps, out_map, pack, unpack, devices, scale)
    back = exchanged_lanes(mix_input, pack, width, devices, me, scale)
    maps = jnp.einsum(
        "cl,glm->gcm", jnp.asarray(unpack, bf16), group_maps, preferred_element_type=f32
    ).astype(bf16)
    grouped = jnp.einsum("rgc,gcm->rgm", back, maps, preferred_element_type=f32).astype(bf16)
    mixed = jnp.dot(
        grouped.reshape(seqs * positions, channels), out_map, preferred_element_type=f32
    )
    return mixed.astype(bf16).reshape(seqs, positions, out_map.shape[1])


def solution(mesh):
    return jax.shard_map(
        per_device,
        mesh=mesh,
        in_specs=(P(None, AXES, None), P(), P()),
        out_specs=P(None, AXES, None),
        check_vma=False,
    )
```

```python
import functools
import math

import jax
import jax.numpy as jnp
import numpy as np
from jax import lax
from jax.experimental import pallas as pl
from jax.experimental.pallas import tpu as pltpu
from jax.sharding import PartitionSpec as P

AXES = ("row", "col")


def turn_tables(left_count, right_count, modulus):
    turns = np.arange(left_count)[:, None] * np.arange(right_count)[None, :] % modulus
    angles = turns * (2.0 * math.pi / modulus)
    return np.cos(angles), np.sin(angles)


def lane_tables(width):
    cosine, sine = turn_tables(width, width, width)
    half = width // 2
    pack = np.zeros((width, width))
    unpack = np.zeros((width, width))
    pack[:, 0::2] = cosine[:, :half]
    pack[:, 1::2] = -sine[:, :half]
    pack[:, 1] = cosine[:, half]
    unpack[0, 0] = 1.0
    unpack[1, half] = 1.0
    for freq in range(1, half):
        unpack[2 * freq, freq] = unpack[2 * freq, width - freq] = 1.0
        unpack[2 * freq + 1, freq] = 1.0
        unpack[2 * freq + 1, width - freq] = -1.0
    return pack, unpack


def fourier(values):
    count = len(values)
    if count == 1:
        return values
    even, odd = fourier(values[0::2]), fourier(values[1::2])
    low, high = [], []
    for at in range(count // 2):
        cosine = math.cos(2.0 * math.pi * at / count)
        sine = math.sin(2.0 * math.pi * at / count)
        (even_re, even_im), (odd_re, odd_im) = even[at], odd[at]
        if at == 0:
            turn_re, turn_im = odd_re, odd_im
        elif 4 * at == count:
            turn_re, turn_im = odd_im, -odd_re
        elif odd_im is None:
            turn_re, turn_im = odd_re * cosine, odd_re * -sine
        else:
            turn_re = odd_re * cosine + odd_im * sine
            turn_im = odd_im * cosine - odd_re * sine
        if turn_re is None:
            low_re = high_re = even_re
        else:
            low_re, high_re = even_re + turn_re, even_re - turn_re
        if turn_im is None:
            low_im = high_im = even_im
        elif even_im is None:
            low_im, high_im = turn_im, -turn_im
        else:
            low_im, high_im = even_im + turn_im, even_im - turn_im
        low.append((low_re, low_im))
        high.append((high_re, high_im))
    return low + high


def mixing_kernel(
    x_hbm, pack_hbm, cos_hbm, sin_hbm, table_hbm, unpack_hbm, given_hbm, outs_hbm,
    out_ref, near, weights,
    x_ref, pack_ref, cos_ref, sin_ref, table_ref, unpack_ref, given_ref, outs_ref, load_sem,
    send, held, stack, big, send_back, back, send_sem, recv_sem, send_back_sem, recv_back_sem,
):
    bf16, f32 = jnp.bfloat16, jnp.float32
    seqs, positions, channels = x_ref.shape
    devices, items, _ = send.shape
    width = pack_ref.shape[0]
    groups = channels // width
    cols = lax.axis_size("col")
    row, col = lax.axis_index("row"), lax.axis_index("col")
    me = row * cols + col
    mesh_ids = pl.DeviceIdType.MESH
    my_y, my_core, my_high = lax.div(row, 2), lax.rem(col, 2), lax.div(col, 4)
    my_x = row - 2 * my_y
    my_low = lax.div(col, 2) - 2 * my_high
    my_inner = my_low + my_high - 2 * my_low * my_high
    members = devices // seqs

    def other(bit, turn):
        return 1 - bit if turn else bit

    def place(x, y, core, low, high):
        inner = low + high - 2 * low * high
        to_row, to_col = y * 2 + x, high * 4 + low * 2 + core
        slot = (2 * core + lax.rem(x + y + low, 2)) * members + to_row * 2 + high
        return to_row, to_col, slot

    my_slot = place(my_x, my_y, my_core, my_low, my_high)[2]
    my_seq = lax.div(my_slot, members)

    far_refs = (pack_hbm, unpack_hbm, given_hbm, outs_hbm, cos_hbm, sin_hbm, table_hbm)
    local_refs = (pack_ref, unpack_ref, given_ref, outs_ref, cos_ref, sin_ref, table_ref)
    x_loads = [
        pltpu.make_async_copy(x_hbm.at[s], x_ref.at[s], load_sem.at[s]) for s in range(seqs)
    ]
    loads = [
        pltpu.make_async_copy(src, dst, load_sem.at[seqs + at])
        for at, (src, dst) in enumerate(zip(far_refs, local_refs))
    ]
    for load in (x_loads[0], loads[0], *x_loads[1:], *loads[1:]):
        load.start()
    barrier = pltpu.get_barrier_semaphore()

    def turned(step):
        bits = [step >> at & 1 for at in range(5)]
        return place(*map(other, (my_x, my_y, my_core, my_low, my_high), bits))

    for step in range(1, devices):
        pl.semaphore_signal(
            barrier, inc=1, device_id=turned(step)[:2], device_id_type=mesh_ids
        )
    rows_t = (((1,), (1,)), ((), ()))

    def slot_copy(src, src_at, dst, dst_at, out_sem, in_sem, where):
        return pltpu.make_async_remote_copy(
            src_ref=src.at[src_at], dst_ref=dst.at[dst_at], send_sem=out_sem, recv_sem=in_sem,
            device_id=where, device_id_type=mesh_ids,
        )

    def several(src, dst, count, out_sem, in_sem):
        return slot_copy(src, pl.ds(0, count), dst, pl.ds(0, count), out_sem, in_sem, (row, col))

    def ready(s):
        x_loads[s].wait()
        for g in range(groups):
            lanes = lax.dot_general(
                pack_ref[...], x_ref[s, :, g * width : (g + 1) * width], rows_t,
                preferred_element_type=f32,
            ).astype(bf16)
            for half in range(2):
                send[(s * groups + g) * 2 + half] = lanes[half * items : (half + 1) * items]

    def send_to(where):
        to_row, to_col, slot = where
        slot_copy(send, slot, held, me, send_sem, recv_sem, (to_row, to_col)).start()

    loads[0].wait()
    for s in range(seqs):
        ready(s)
        if s == 0:
            pl.semaphore_wait(barrier, devices - 1)
        for step in range(members - 1, -1, -1):
            x, y, high = (other(bit, step >> at & 1) for at, bit in enumerate((my_x, my_y, my_high)))
            low = lax.rem(s % 2 + x + y, 2)
            where = place(x, y, s // 2, low, high)
            if step == 0:
                @pl.when(my_seq != s)
                def _():
                    send_to(where)
            else:
                send_to(where)

    held[me] = send[my_slot]

    for load in loads[1:4]:
        load.wait()
    for g in range(groups):
        rows = slice(g * width, (g + 1) * width)
        maps = jnp.dot(unpack_ref[...], given_ref[g], preferred_element_type=f32).astype(bf16)
        weights[rows, :] = jnp.dot(
            maps, outs_ref[rows, :], preferred_element_type=f32
        ).astype(bf16)
    for load in loads[4:]:
        load.wait()
    several(send, held, devices - 1, send_sem, recv_sem).wait_recv()

    tile = 16
    def spin(chunk, carry):
        rows = pl.ds(pl.multiple_of(chunk * tile, tile), tile)
        spun = fourier([(held[d, rows, :].astype(f32), None) for d in range(devices)])
        row_ids = chunk * tile + lax.broadcasted_iota(jnp.int32, (tile, positions), 0)
        lane_ids = lax.rem(my_slot * items + row_ids, width)
        is_sine = (lax.rem(lane_ids, 2) == 1) & (lane_ids != 1)
        for f in range(devices):
            real_in, imag_in = spun[f]
            cosine, sine = cos_ref[f : f + 1, :], sin_ref[f : f + 1, :]
            if imag_in is None:
                real_part, imag_part = real_in * cosine, -(real_in * sine)
            else:
                real_part = real_in * cosine + imag_in * sine
                imag_part = imag_in * cosine - real_in * sine
            stack[f, rows, :positions] = jnp.where(is_sine, -imag_part, real_part).astype(bf16)
            stack[f, rows, positions:] = jnp.where(is_sine, real_part, imag_part).astype(bf16)
        return carry

    lax.fori_loop(0, items // tile, spin, 0)
    pairs = devices // 2
    for a in range(pairs):
        both = jnp.concatenate([stack[a], stack[a + pairs]], axis=0)
        big[pl.ds(a, positions, stride=pairs), :] = lax.dot_general(
            table_ref[...], both, rows_t, preferred_element_type=f32
        )
    for e in range(devices):
        send_back[e] = big[e * items : (e + 1) * items, :].astype(bf16)

    for step in range(1, devices):
        to_row, to_col, _ = turned(step)
        slot_copy(
            send_back, to_row * cols + to_col, back, my_slot, send_back_sem,
            recv_back_sem.at[my_seq], (to_row, to_col),
        ).start()
    back[my_slot] = send_back[me]
    several(send, held, devices - 1, send_sem, recv_sem).wait_send()

    left = lax.broadcasted_iota(jnp.int32, (items, width), 1) < items

    def gather(s):
        @pl.when(my_seq == s)
        def _():
            several(send_back, back, members - 1, send_back_sem, recv_back_sem.at[s]).wait_recv()

        @pl.when(my_seq != s)
        def _():
            several(send_back, back, members, send_back_sem, recv_back_sem.at[s]).wait_recv()

        for g in range(groups):
            slot = s * members + g * 2
            first, second = back[slot].astype(f32), back[slot + 1].astype(f32)
            lanes = slice(g * width, (g + 1) * width)
            near[:items, lanes] = jnp.where(left, first, pltpu.roll(second, items, 1)).astype(bf16)
            near[items:, lanes] = jnp.where(left, pltpu.roll(first, items, 1), second).astype(bf16)

    def finish(s, carry):
        gather(s)
        product(near, weights, out_ref.at[s], devices)
        return carry

    lax.fori_loop(0, seqs - 1, finish, 0)
    gather(seqs - 1)
    several(send_back, back, devices - 1, send_back_sem, recv_back_sem.at[0]).wait_send()


CHUNK = 512


def product(near, weights, out_ref, devices, done=None):
    positions = near.shape[0]
    items, pairs = positions // 2, devices // 2
    for at in range(0, weights.shape[1], CHUNK):
        made = jnp.dot(
            near[...], weights[:, at : at + CHUNK], preferred_element_type=jnp.float32
        ).astype(jnp.bfloat16)
        for h in range(2):
            for m in range(items // pairs):
                base, had = m * devices + h * pairs, h * items + m * pairs
                out_ref[base : base + pairs, at : at + CHUNK] = made[had : had + pairs]
        if done is not None:
            done(at)


def last_kernel(devices, early, near, weights, out_hbm, late, early_sem, late_sem):
    seqs = early.shape[0] + 1
    early_copies = [
        pltpu.make_async_copy(early.at[s], out_hbm.at[s], early_sem.at[s]) for s in range(seqs - 1)
    ]
    for copy in early_copies:
        copy.start()
    late_copies = []

    def done(at):
        lanes = pl.ds(at, CHUNK)
        copy = pltpu.make_async_copy(
            late.at[:, lanes], out_hbm.at[seqs - 1, :, lanes], late_sem.at[at // CHUNK]
        )
        copy.start()
        late_copies.append(copy)

    product(near, weights, late, devices, done)
    for copy in early_copies + late_copies:
        copy.wait()


def fused_lanes(mix_input, group_maps, out_map, pack, unpack, devices, scale):
    bf16, f32 = jnp.bfloat16, jnp.float32
    seqs, positions, channels = mix_input.shape
    width = pack.shape[0]
    items = seqs * channels // devices
    length = devices * positions
    twist_cos, twist_sin = turn_tables(devices, positions, length)
    pos_cos, pos_sin = turn_tables(positions, positions, positions)
    table = np.concatenate([pos_cos, pos_sin], axis=1) * scale
    slots = (devices, items, positions)
    hbm = pl.BlockSpec(memory_space=pltpu.HBM)
    dma = pltpu.SemaphoreType.DMA
    vmem = pl.BlockSpec(memory_space=pltpu.VMEM)
    model = out_map.shape[1]
    given = (
        mix_input, jnp.asarray(pack.T, bf16), jnp.asarray(twist_cos, f32),
        jnp.asarray(twist_sin, f32), jnp.asarray(table, bf16), jnp.asarray(unpack, bf16), group_maps,
        out_map,
    )
    early, near, weights = pl.pallas_call(
        mixing_kernel,
        out_shape=[
            pltpu.VMEM((seqs - 1, positions, model), bf16), pltpu.VMEM((positions, channels), bf16),
            pltpu.VMEM(out_map.shape, bf16),
        ],
        in_specs=[hbm] * 8,
        out_specs=[vmem] * 3,
        scratch_shapes=[
            pltpu.VMEM(mix_input.shape, bf16), pltpu.VMEM(pack.shape, bf16),
            pltpu.VMEM(twist_cos.shape, f32), pltpu.VMEM(twist_sin.shape, f32),
            pltpu.VMEM(table.shape, bf16), pltpu.VMEM(unpack.shape, bf16),
            pltpu.VMEM(group_maps.shape, bf16), pltpu.VMEM(out_map.shape, bf16), dma((seqs + 7,)),
            pltpu.VMEM(slots, bf16), pltpu.VMEM(slots, bf16),
            pltpu.VMEM((devices, items, 2 * positions), bf16),
            pltpu.VMEM((devices * items, width), f32),
            pltpu.VMEM(slots, bf16), pltpu.VMEM(slots, bf16),
            dma, dma, dma, dma((seqs,)),
        ],
        compiler_params=pltpu.CompilerParams(
            collective_id=0, has_side_effects=True, vmem_limit_bytes=32 << 20
        ),
    )(*(pltpu.with_memory_space_constraint(value, pltpu.HBM) for value in given))
    kept = [pltpu.with_memory_space_constraint(value, pltpu.VMEM) for value in (early, near, weights)]
    return pl.pallas_call(
        functools.partial(last_kernel, devices),
        out_shape=jax.ShapeDtypeStruct((seqs, positions, model), bf16),
        in_specs=[vmem] * 3,
        out_specs=hbm,
        scratch_shapes=[
            pltpu.VMEM((positions, model), bf16), dma((seqs - 1,)), dma((model // CHUNK,)),
        ],
        compiler_params=pltpu.CompilerParams(vmem_limit_bytes=16 << 20),
    )(*kept)


def exchanged_lanes(mix_input, pack, width, devices, me, scale):
    bf16, f32 = jnp.bfloat16, jnp.float32
    seqs, positions, channels = mix_input.shape
    groups = channels // width
    length = devices * positions
    items = seqs * channels // devices
    lanes = jnp.einsum(
        "spgj,jc->sgcp",
        mix_input.reshape(seqs, positions, groups, width),
        jnp.asarray(pack, bf16),
        preferred_element_type=f32,
    ).astype(bf16)
    sent = lanes.reshape(devices, items, positions)
    held = lax.all_to_all(sent, AXES, split_axis=0, concat_axis=0, tiled=True)

    dev_cos, dev_sin = turn_tables(devices, devices, devices)
    both = jnp.asarray(np.concatenate([dev_cos, -dev_sin], axis=1), bf16)
    spun = jnp.einsum("df,dnp->fnp", both, held, preferred_element_type=f32)
    real_in, imag_in = spun[:devices], spun[devices:]
    twist_cos, twist_sin = turn_tables(devices, positions, length)
    twist_cos = jnp.asarray(twist_cos, f32)[:, None, :]
    twist_sin = jnp.asarray(twist_sin, f32)[:, None, :]
    real_part = real_in * twist_cos + imag_in * twist_sin
    imag_part = imag_in * twist_cos - real_in * twist_sin
    lane_ids = (me * items + jnp.arange(items, dtype=jnp.int32)) % width
    is_sine = ((lane_ids % 2 == 1) & (lane_ids != 1))[None, :, None]
    first = jnp.where(is_sine, -imag_part, real_part).astype(bf16)
    second = jnp.where(is_sine, real_part, imag_part).astype(bf16)
    stacked = jnp.concatenate([first, second], axis=2)
    pos_cos, pos_sin = turn_tables(positions, positions, positions)
    pos_table = jnp.asarray(np.concatenate([pos_cos, pos_sin], axis=0) * scale, bf16)
    freqs = jnp.einsum("pm,fnp->mfn", pos_table, stacked, preferred_element_type=f32).astype(bf16)

    freqs = freqs.reshape(devices, positions, items)
    back = lax.all_to_all(freqs, AXES, split_axis=0, concat_axis=0, tiled=True)
    parts = width // items
    back = back.reshape(seqs, groups, parts, positions, items)
    return back.transpose(0, 3, 1, 2, 4).reshape(seqs * positions, groups, width)


def per_device(mix_input, group_maps, out_map):
    bf16, f32 = jnp.bfloat16, jnp.float32
    seqs, positions, channels = mix_input.shape
    groups, width, _ = group_maps.shape
    devices = lax.axis_size("row") * lax.axis_size("col")
    me = lax.axis_index("row") * lax.axis_size("col") + lax.axis_index("col")
    items = seqs * channels // devices
    pack, unpack = lane_tables(width)
    scale = 1.0 / math.sqrt(devices * positions * width)
    square = 2 * items == width and positions == width and items == 2 * devices
    if square and lax.axis_size("col") == 8 and seqs == 4:
        return fused_lanes(mix_input, group_maps, out_map, pack, unpack, devices, scale)
    back = exchanged_lanes(mix_input, pack, width, devices, me, scale)
    maps = jnp.einsum(
        "cl,glm->gcm", jnp.asarray(unpack, bf16), group_maps, preferred_element_type=f32
    ).astype(bf16)
    grouped = jnp.einsum("rgc,gcm->rgm", back, maps, preferred_element_type=f32).astype(bf16)
    mixed = jnp.dot(
        grouped.reshape(seqs * positions, channels), out_map, preferred_element_type=f32
    )
    return mixed.astype(bf16).reshape(seqs, positions, out_map.shape[1])


def solution(mesh):
    return jax.shard_map(
        per_device,
        mesh=mesh,
        in_specs=(P(None, AXES, None), P(), P()),
        out_specs=P(None, AXES, None),
        check_vma=False,
    )
```

```python
import functools
import math

import jax
import jax.numpy as jnp
import numpy as np
from jax import lax
from jax.experimental import pallas as pl
from jax.experimental.pallas import tpu as pltpu
from jax.sharding import PartitionSpec as P

AXES = ("row", "col")


def turn_tables(left_count, right_count, modulus):
    turns = np.arange(left_count)[:, None] * np.arange(right_count)[None, :] % modulus
    angles = turns * (2.0 * math.pi / modulus)
    return np.cos(angles), np.sin(angles)


def lane_tables(width):
    cosine, sine = turn_tables(width, width, width)
    half = width // 2
    pack = np.zeros((width, width))
    unpack = np.zeros((width, width))
    pack[:, 0::2] = cosine[:, :half]
    pack[:, 1::2] = -sine[:, :half]
    pack[:, 1] = cosine[:, half]
    unpack[0, 0] = 1.0
    unpack[1, half] = 1.0
    for freq in range(1, half):
        unpack[2 * freq, freq] = unpack[2 * freq, width - freq] = 1.0
        unpack[2 * freq + 1, freq] = 1.0
        unpack[2 * freq + 1, width - freq] = -1.0
    return pack, unpack


def fourier(values):
    count = len(values)
    if count == 1:
        return [(values[0], None)]
    if count == 2:
        return [(values[0] + values[1], None), (values[0] - values[1], None)]
    even, odd = fourier(values[0::2]), fourier(values[1::2])
    low, high = [], []
    for at in range(count // 4 + 1):
        (even_re, even_im), (odd_re, odd_im) = even[at], odd[at]
        if at == 0:
            low.append((even_re + odd_re, None))
            high.append((even_re - odd_re, None))
        elif 4 * at == count:
            low.append((even_re, -odd_re))
        else:
            cosine = math.cos(2.0 * math.pi * at / count)
            sine = math.sin(2.0 * math.pi * at / count)
            turn_re = odd_re * cosine + odd_im * sine
            turn_im = odd_im * cosine - odd_re * sine
            low.append((even_re + turn_re, even_im + turn_im))
            high.append((even_re - turn_re, turn_im - even_im))
    return low + high[::-1]


def mixing_kernel(
    x_hbm, pack_hbm, cos_hbm, sin_hbm, table_hbm, unpack_hbm, given_hbm, outs_hbm,
    out_ref, near, weights,
    x_ref, pack_ref, cos_ref, sin_ref, table_ref, unpack_ref, given_ref, outs_ref, load_sem,
    send, held, stack, big, send_back, back, send_sem, recv_sem, send_back_sem, recv_back_sem,
    twist_a, twist_b,
):
    bf16, f32 = jnp.bfloat16, jnp.float32
    seqs, positions, channels = x_ref.shape
    devices, items, _ = send.shape
    width = pack_ref.shape[0]
    groups = channels // width
    cols = lax.axis_size("col")
    row, col = lax.axis_index("row"), lax.axis_index("col")
    me = row * cols + col
    mesh_ids = pl.DeviceIdType.MESH
    my_y, my_core, my_high = lax.div(row, 2), lax.rem(col, 2), lax.div(col, 4)
    my_x = row - 2 * my_y
    my_low = lax.div(col, 2) - 2 * my_high
    my_inner = my_low + my_high - 2 * my_low * my_high
    members = devices // seqs

    def other(bit, turn):
        return 1 - bit if turn else bit

    def place(x, y, core, low, high):
        inner = low + high - 2 * low * high
        to_row, to_col = y * 2 + x, high * 4 + low * 2 + core
        slot = (2 * core + lax.rem(x + y + low, 2)) * members + to_row * 2 + high
        return to_row, to_col, slot

    my_slot = place(my_x, my_y, my_core, my_low, my_high)[2]
    my_seq = lax.div(my_slot, members)

    far_refs = (pack_hbm, unpack_hbm, given_hbm, outs_hbm, cos_hbm, sin_hbm, table_hbm)
    local_refs = (pack_ref, unpack_ref, given_ref, outs_ref, cos_ref, sin_ref, table_ref)
    x_loads = [
        pltpu.make_async_copy(x_hbm.at[s], x_ref.at[s], load_sem.at[s]) for s in range(seqs)
    ]
    loads = [
        pltpu.make_async_copy(src, dst, load_sem.at[seqs + at])
        for at, (src, dst) in enumerate(zip(far_refs, local_refs))
    ]
    for load in (x_loads[0], loads[0], *x_loads[1:], *loads[1:]):
        load.start()
    barrier = pltpu.get_barrier_semaphore()

    def turned(step):
        bits = [step >> at & 1 for at in range(5)]
        return place(*map(other, (my_x, my_y, my_core, my_low, my_high), bits))

    for step in range(1, devices):
        pl.semaphore_signal(
            barrier, inc=1, device_id=turned(step)[:2], device_id_type=mesh_ids
        )
    rows_t = (((1,), (1,)), ((), ()))

    def slot_copy(src, src_at, dst, dst_at, out_sem, in_sem, where):
        return pltpu.make_async_remote_copy(
            src_ref=src.at[src_at], dst_ref=dst.at[dst_at], send_sem=out_sem, recv_sem=in_sem,
            device_id=where, device_id_type=mesh_ids,
        )

    def several(src, dst, count, out_sem, in_sem):
        return slot_copy(src, pl.ds(0, count), dst, pl.ds(0, count), out_sem, in_sem, (row, col))

    def ready(s):
        x_loads[s].wait()
        for g in range(groups):
            lanes = lax.dot_general(
                pack_ref[...], x_ref[s, :, g * width : (g + 1) * width], rows_t,
                preferred_element_type=f32,
            ).astype(bf16)
            for half in range(2):
                send[(s * groups + g) * 2 + half] = lanes[half * items : (half + 1) * items]

    def send_to(where):
        to_row, to_col, slot = where
        slot_copy(send, slot, held, me, send_sem, recv_sem, (to_row, to_col)).start()

    loads[0].wait()
    for s in range(seqs):
        ready(s)
        if s == 0:
            pl.semaphore_wait(barrier, devices - 1)
        for turn_high, outer, turn_x in ((1, 1, 1), (1, 1, 0), (1, 0, 1), (1, 0, 0), (0, 0, 1), (0, 0, 0), (0, 1, 1), (0, 1, 0)):
            x, high = other(my_x, turn_x), other(my_high, turn_high)
            kind = lax.rem(s + high + outer, 2)
            y = x + kind - 2 * x * kind
            where = place(x, y, s // 2, lax.rem(s % 2 + x + y, 2), high)
            if turn_high or turn_x:
                send_to(where)
            else:
                @pl.when(where[0] * cols + where[1] != me)
                def _():
                    send_to(where)
    held[me] = send[my_slot]

    for load in loads[1:4]:
        load.wait()
    for g in range(groups):
        rows = slice(g * width, (g + 1) * width)
        maps = jnp.dot(unpack_ref[...], given_ref[g], preferred_element_type=f32).astype(bf16)
        weights[rows, :] = jnp.dot(
            maps, outs_ref[rows, :], preferred_element_type=f32
        ).astype(bf16)
    for load in loads[4:]:
        load.wait()
    tile = twist_a.shape[2]
    row_ids = lax.broadcasted_iota(jnp.int32, (tile, positions), 0)
    for kind in range(2):
        is_sine = lax.rem(row_ids, 2) == 1
        if kind == 1:
            is_sine = is_sine & (row_ids != 1)
        for f in range(devices):
            cosine, sine = cos_ref[f : f + 1, :], sin_ref[f : f + 1, :]
            twist_a[kind, f] = jnp.where(is_sine, sine, cosine)
            twist_b[kind, f] = jnp.where(is_sine, -cosine, sine)
    several(send, held, devices - 1, send_sem, recv_sem).wait_recv()

    def spin(chunk, carry):
        rows = pl.ds(pl.multiple_of(chunk * tile, tile), tile)
        kind = jnp.where((chunk == 0) & (lax.rem(my_slot, 2) == 0), 1, 0)
        spun = fourier([held[d, rows, :].astype(f32) for d in range(devices)])
        for f in range(devices):
            real, imag = spun[min(f, devices - f)]
            turn_a, turn_b = twist_a[kind, f], twist_b[kind, f]
            if imag is None:
                first, second = real * turn_a, -(real * turn_b)
            elif 2 * f < devices:
                first, second = real * turn_a + imag * turn_b, imag * turn_a - real * turn_b
            else:
                first, second = real * turn_a - imag * turn_b, -(imag * turn_a + real * turn_b)
            stack[f, rows, :positions] = first.astype(bf16)
            stack[f, rows, positions:] = second.astype(bf16)
        return carry

    lax.fori_loop(0, items // tile, spin, 0)
    pairs = devices // 2
    for a in range(0, pairs, 2):
        both = jnp.concatenate(
            [stack[a], stack[a + pairs], stack[a + 1], stack[a + 1 + pairs]], axis=0
        )
        made = lax.dot_general(table_ref[...], both, rows_t, preferred_element_type=f32)
        big[pl.ds(a, positions, stride=pairs), :] = made[:, :width]
        big[pl.ds(a + 1, positions, stride=pairs), :] = made[:, width:]
    for e in range(devices):
        send_back[e] = big[e * items : (e + 1) * items, :].astype(bf16)

    def back_to(where, first):
        to_row, to_col, _ = where

        def go():
            slot_copy(
                send_back, to_row * cols + to_col, back, my_slot, send_back_sem,
                recv_back_sem.at[my_seq], (to_row, to_col),
            ).start()

        at = to_row * cols + to_col
        if first:
            pl.when(at != me)(go)
        else:
            pl.when((at != me) & (at >= 2))(go)

    for core in range(2):
        back_to((0, core, None), True)
    for level, step, core in ((0, 3, 0), (0, 2, 0), (0, 3, 1), (0, 2, 1), (0, 1, 0), (0, 0, 0), (0, 1, 1), (0, 0, 1), (1, 3, 0), (1, 2, 0), (1, 3, 1), (1, 2, 1), (1, 1, 0), (1, 0, 0), (1, 1, 1), (1, 0, 1), (2, 3, 0), (2, 2, 0), (2, 3, 1), (2, 2, 1), (2, 1, 0), (2, 0, 0), (2, 1, 1), (2, 0, 1), (3, 3, 0), (3, 2, 0), (3, 3, 1), (3, 2, 1), (3, 1, 0), (3, 0, 0), (3, 1, 1), (3, 0, 1)):
        x, y = other(my_x, step & 1), other(my_y, step >> 1)
        back_to(place(x, y, core, level % 2, level // 2), False)

    back[my_slot] = send_back[me]
    several(send, held, devices - 1, send_sem, recv_sem).wait_send()

    left = lax.broadcasted_iota(jnp.int32, (items, width), 1) < items

    def gather(s):
        @pl.when(my_seq == s)
        def _():
            several(send_back, back, members - 1, send_back_sem, recv_back_sem.at[s]).wait_recv()

        @pl.when(my_seq != s)
        def _():
            several(send_back, back, members, send_back_sem, recv_back_sem.at[s]).wait_recv()

        for g in range(groups):
            slot = s * members + g * 2
            first, second = back[slot].astype(f32), back[slot + 1].astype(f32)
            lanes = slice(g * width, (g + 1) * width)
            near[:items, lanes] = jnp.where(left, first, pltpu.roll(second, items, 1)).astype(bf16)
            near[items:, lanes] = jnp.where(left, pltpu.roll(first, items, 1), second).astype(bf16)

    def finish(s, carry):
        gather(s)
        product(near, weights, out_ref.at[s], devices)
        return carry

    lax.fori_loop(0, seqs - 1, finish, 0)
    gather(seqs - 1)
    several(send_back, back, devices - 1, send_back_sem, recv_back_sem.at[0]).wait_send()


CHUNK = 512


def product(near, weights, out_ref, devices, done=None):
    positions = near.shape[0]
    items, pairs = positions // 2, devices // 2
    for at in range(0, weights.shape[1], CHUNK):
        made = jnp.dot(
            near[...], weights[:, at : at + CHUNK], preferred_element_type=jnp.float32
        ).astype(jnp.bfloat16)
        for h in range(2):
            for m in range(items // pairs):
                base, had = m * devices + h * pairs, h * items + m * pairs
                out_ref[base : base + pairs, at : at + CHUNK] = made[had : had + pairs]
        if done is not None:
            done(at)


def last_kernel(devices, early, near, weights, out_hbm, late, early_sem, late_sem):
    seqs = early.shape[0] + 1
    early_copies = [
        pltpu.make_async_copy(early.at[s], out_hbm.at[s], early_sem.at[s]) for s in range(seqs - 1)
    ]
    for copy in early_copies:
        copy.start()
    late_copies = []

    def done(at):
        lanes = pl.ds(at, CHUNK)
        copy = pltpu.make_async_copy(
            late.at[:, lanes], out_hbm.at[seqs - 1, :, lanes], late_sem.at[at // CHUNK]
        )
        copy.start()
        late_copies.append(copy)

    product(near, weights, late, devices, done)
    for copy in early_copies + late_copies:
        copy.wait()


def fused_lanes(mix_input, group_maps, out_map, pack, unpack, devices, scale):
    bf16, f32 = jnp.bfloat16, jnp.float32
    seqs, positions, channels = mix_input.shape
    width = pack.shape[0]
    items = seqs * channels // devices
    length = devices * positions
    twist_cos, twist_sin = turn_tables(devices, positions, length)
    pos_cos, pos_sin = turn_tables(positions, positions, positions)
    table = np.concatenate([pos_cos, pos_sin], axis=1) * scale
    slots = (devices, items, positions)
    hbm = pl.BlockSpec(memory_space=pltpu.HBM)
    dma = pltpu.SemaphoreType.DMA
    vmem = pl.BlockSpec(memory_space=pltpu.VMEM)
    model = out_map.shape[1]
    given = (
        mix_input, jnp.asarray(pack.T, bf16), jnp.asarray(twist_cos, f32),
        jnp.asarray(twist_sin, f32), jnp.asarray(table, bf16), jnp.asarray(unpack, bf16), group_maps,
        out_map,
    )
    early, near, weights = pl.pallas_call(
        mixing_kernel,
        out_shape=[
            pltpu.VMEM((seqs - 1, positions, model), bf16), pltpu.VMEM((positions, channels), bf16),
            pltpu.VMEM(out_map.shape, bf16),
        ],
        in_specs=[hbm] * 8,
        out_specs=[vmem] * 3,
        scratch_shapes=[
            pltpu.VMEM(mix_input.shape, bf16), pltpu.VMEM(pack.shape, bf16),
            pltpu.VMEM(twist_cos.shape, f32), pltpu.VMEM(twist_sin.shape, f32),
            pltpu.VMEM(table.shape, bf16), pltpu.VMEM(unpack.shape, bf16),
            pltpu.VMEM(group_maps.shape, bf16), pltpu.VMEM(out_map.shape, bf16), dma((seqs + 7,)),
            pltpu.VMEM(slots, bf16), pltpu.VMEM(slots, bf16),
            pltpu.VMEM((devices, items, 2 * positions), bf16),
            pltpu.VMEM((devices * items, width), f32),
            pltpu.VMEM(slots, bf16), pltpu.VMEM(slots, bf16),
            dma, dma, dma, dma((seqs,)),
            pltpu.VMEM((2, devices, 16, positions), f32), pltpu.VMEM((2, devices, 16, positions), f32),
        ],
        compiler_params=pltpu.CompilerParams(
            collective_id=0, has_side_effects=True, vmem_limit_bytes=32 << 20
        ),
    )(*(pltpu.with_memory_space_constraint(value, pltpu.HBM) for value in given))
    kept = [pltpu.with_memory_space_constraint(value, pltpu.VMEM) for value in (early, near, weights)]
    return pl.pallas_call(
        functools.partial(last_kernel, devices),
        out_shape=jax.ShapeDtypeStruct((seqs, positions, model), bf16),
        in_specs=[vmem] * 3,
        out_specs=hbm,
        scratch_shapes=[
            pltpu.VMEM((positions, model), bf16), dma((seqs - 1,)), dma((model // CHUNK,)),
        ],
        compiler_params=pltpu.CompilerParams(vmem_limit_bytes=16 << 20),
    )(*kept)


def exchanged_lanes(mix_input, pack, width, devices, me, scale):
    bf16, f32 = jnp.bfloat16, jnp.float32
    seqs, positions, channels = mix_input.shape
    groups = channels // width
    length = devices * positions
    items = seqs * channels // devices
    lanes = jnp.einsum(
        "spgj,jc->sgcp",
        mix_input.reshape(seqs, positions, groups, width),
        jnp.asarray(pack, bf16),
        preferred_element_type=f32,
    ).astype(bf16)
    sent = lanes.reshape(devices, items, positions)
    held = lax.all_to_all(sent, AXES, split_axis=0, concat_axis=0, tiled=True)

    dev_cos, dev_sin = turn_tables(devices, devices, devices)
    both = jnp.asarray(np.concatenate([dev_cos, -dev_sin], axis=1), bf16)
    spun = jnp.einsum("df,dnp->fnp", both, held, preferred_element_type=f32)
    real_in, imag_in = spun[:devices], spun[devices:]
    twist_cos, twist_sin = turn_tables(devices, positions, length)
    twist_cos = jnp.asarray(twist_cos, f32)[:, None, :]
    twist_sin = jnp.asarray(twist_sin, f32)[:, None, :]
    real_part = real_in * twist_cos + imag_in * twist_sin
    imag_part = imag_in * twist_cos - real_in * twist_sin
    lane_ids = (me * items + jnp.arange(items, dtype=jnp.int32)) % width
    is_sine = ((lane_ids % 2 == 1) & (lane_ids != 1))[None, :, None]
    first = jnp.where(is_sine, -imag_part, real_part).astype(bf16)
    second = jnp.where(is_sine, real_part, imag_part).astype(bf16)
    stacked = jnp.concatenate([first, second], axis=2)
    pos_cos, pos_sin = turn_tables(positions, positions, positions)
    pos_table = jnp.asarray(np.concatenate([pos_cos, pos_sin], axis=0) * scale, bf16)
    freqs = jnp.einsum("pm,fnp->mfn", pos_table, stacked, preferred_element_type=f32).astype(bf16)

    freqs = freqs.reshape(devices, positions, items)
    back = lax.all_to_all(freqs, AXES, split_axis=0, concat_axis=0, tiled=True)
    parts = width // items
    back = back.reshape(seqs, groups, parts, positions, items)
    return back.transpose(0, 3, 1, 2, 4).reshape(seqs * positions, groups, width)


def per_device(mix_input, group_maps, out_map):
    bf16, f32 = jnp.bfloat16, jnp.float32
    seqs, positions, channels = mix_input.shape
    groups, width, _ = group_maps.shape
    devices = lax.axis_size("row") * lax.axis_size("col")
    me = lax.axis_index("row") * lax.axis_size("col") + lax.axis_index("col")
    items = seqs * channels // devices
    pack, unpack = lane_tables(width)
    scale = 1.0 / math.sqrt(devices * positions * width)
    square = 2 * items == width and positions == width and items == 2 * devices
    if square and lax.axis_size("col") == 8 and seqs == 4:
        return fused_lanes(mix_input, group_maps, out_map, pack, unpack, devices, scale)
    back = exchanged_lanes(mix_input, pack, width, devices, me, scale)
    maps = jnp.einsum(
        "cl,glm->gcm", jnp.asarray(unpack, bf16), group_maps, preferred_element_type=f32
    ).astype(bf16)
    grouped = jnp.einsum("rgc,gcm->rgm", back, maps, preferred_element_type=f32).astype(bf16)
    mixed = jnp.dot(
        grouped.reshape(seqs * positions, channels), out_map, preferred_element_type=f32
    )
    return mixed.astype(bf16).reshape(seqs, positions, out_map.shape[1])


def solution(mesh):
    return jax.shard_map(
        per_device,
        mesh=mesh,
        in_specs=(P(None, AXES, None), P(), P()),
        out_specs=P(None, AXES, None),
        check_vma=False,
    )
```

```python
import functools
import math

import jax
import jax.numpy as jnp
import numpy as np
from jax import lax
from jax.experimental import pallas as pl
from jax.experimental.pallas import tpu as pltpu
from jax.sharding import PartitionSpec as P

AXES = ("row", "col")


def turn_tables(left_count, right_count, modulus):
    turns = np.arange(left_count)[:, None] * np.arange(right_count)[None, :] % modulus
    angles = turns * (2.0 * math.pi / modulus)
    return np.cos(angles), np.sin(angles)


def lane_tables(width):
    cosine, sine = turn_tables(width, width, width)
    half = width // 2
    pack = np.zeros((width, width))
    unpack = np.zeros((width, width))
    pack[:, 0::2] = cosine[:, :half]
    pack[:, 1::2] = -sine[:, :half]
    pack[:, 1] = cosine[:, half]
    unpack[0, 0] = 1.0
    unpack[1, half] = 1.0
    for freq in range(1, half):
        unpack[2 * freq, freq] = unpack[2 * freq, width - freq] = 1.0
        unpack[2 * freq + 1, freq] = 1.0
        unpack[2 * freq + 1, width - freq] = -1.0
    return pack, unpack


def fourier(values):
    count = len(values)
    if count == 1:
        return [(values[0], None)]
    if count == 2:
        return [(values[0] + values[1], None), (values[0] - values[1], None)]
    even, odd = fourier(values[0::2]), fourier(values[1::2])
    low, high = [], []
    for at in range(count // 4 + 1):
        (even_re, even_im), (odd_re, odd_im) = even[at], odd[at]
        if at == 0:
            low.append((even_re + odd_re, None))
            high.append((even_re - odd_re, None))
        elif 4 * at == count:
            low.append((even_re, -odd_re))
        else:
            cosine = math.cos(2.0 * math.pi * at / count)
            sine = math.sin(2.0 * math.pi * at / count)
            turn_re = odd_re * cosine + odd_im * sine
            turn_im = odd_im * cosine - odd_re * sine
            low.append((even_re + turn_re, even_im + turn_im))
            high.append((even_re - turn_re, turn_im - even_im))
    return low + high[::-1]


def mixing_kernel(
    x_hbm, pack_hbm, cos_hbm, sin_hbm, table_hbm, unpack_hbm, given_hbm, outs_hbm,
    out_ref, near, weights,
    x_ref, pack_ref, cos_ref, sin_ref, table_ref, unpack_ref, given_ref, outs_ref, load_sem,
    send, held, stack, big, send_back, back, send_sem, recv_sem, send_back_sem, recv_back_sem,
    twist_a, twist_b, ends,
):
    bf16, f32 = jnp.bfloat16, jnp.float32
    seqs, positions, channels = x_ref.shape
    devices, items, _ = send.shape
    width = pack_ref.shape[0]
    groups = channels // width
    cols = lax.axis_size("col")
    row, col = lax.axis_index("row"), lax.axis_index("col")
    me = row * cols + col
    mesh_ids = pl.DeviceIdType.MESH
    my_y, my_core, my_high = lax.div(row, 2), lax.rem(col, 2), lax.div(col, 4)
    my_x = row - 2 * my_y
    my_low = lax.div(col, 2) - 2 * my_high
    my_inner = my_low + my_high - 2 * my_low * my_high
    members = devices // seqs

    def other(bit, turn):
        return 1 - bit if turn else bit

    def place(x, y, core, low, high):
        inner = low + high - 2 * low * high
        to_row, to_col = y * 2 + x, high * 4 + low * 2 + core
        slot = (2 * core + lax.rem(x + y + low, 2)) * members + to_row * 2 + high
        return to_row, to_col, slot

    my_slot = place(my_x, my_y, my_core, my_low, my_high)[2]
    my_seq = lax.div(my_slot, members)

    far_refs = (pack_hbm, unpack_hbm, given_hbm, outs_hbm, cos_hbm, sin_hbm, table_hbm)
    local_refs = (pack_ref, unpack_ref, given_ref, outs_ref, cos_ref, sin_ref, table_ref)
    x_loads = [
        pltpu.make_async_copy(x_hbm.at[s], x_ref.at[s], load_sem.at[s]) for s in range(seqs)
    ]
    loads = [
        pltpu.make_async_copy(src, dst, load_sem.at[seqs + at])
        for at, (src, dst) in enumerate(zip(far_refs, local_refs))
    ]
    for load in (x_loads[0], loads[0], *x_loads[1:], *loads[1:]):
        load.start()
    barrier = pltpu.get_barrier_semaphore()

    def turned(step):
        bits = [step >> at & 1 for at in range(5)]
        return place(*map(other, (my_x, my_y, my_core, my_low, my_high), bits))

    def tell(sem, steps):
        for step in steps:
            pl.semaphore_signal(
                sem, inc=1, device_id=turned(step)[:2], device_id_type=mesh_ids
            )

    same_kind = [step for step in range(1, devices) if step // 8 in (0, 3)]
    other_kind = [step for step in range(1, devices) if step // 8 in (1, 2)]
    tell(barrier, same_kind)

    @pl.when(my_inner == 1)
    def _():
        tell(barrier, other_kind)

    rows_t = (((1,), (1,)), ((), ()))

    def slot_copy(src, src_at, dst, dst_at, out_sem, in_sem, where):
        return pltpu.make_async_remote_copy(
            src_ref=src.at[src_at], dst_ref=dst.at[dst_at], send_sem=out_sem, recv_sem=in_sem,
            device_id=where, device_id_type=mesh_ids,
        )

    def several(src, dst, count, out_sem, in_sem):
        return slot_copy(src, pl.ds(0, count), dst, pl.ds(0, count), out_sem, in_sem, (row, col))

    def ready(s):
        x_loads[s].wait()
        for g in range(groups):
            lanes = lax.dot_general(
                pack_ref[...], x_ref[s, :, g * width : (g + 1) * width], rows_t,
                preferred_element_type=f32,
            ).astype(bf16)
            for half in range(2):
                send[(s * groups + g) * 2 + half] = lanes[half * items : (half + 1) * items]

    def send_to(where):
        to_row, to_col, slot = where
        slot_copy(send, slot, held, me, send_sem, recv_sem, (to_row, to_col)).start()

    def first_of(s, turn_high, outer, turn_x):
        x, high = other(my_x, turn_x), other(my_high, turn_high)
        kind = lax.rem(s + high + outer, 2)
        y = x + kind - 2 * x * kind
        return place(x, y, s // 2, lax.rem(s % 2 + x + y, 2), high)

    def send_but_me(where):
        @pl.when(where[0] * cols + where[1] != me)
        def _():
            send_to(where)

    def to_end(s, high):
        for turn_x in (1, 0):
            x = other(my_x, turn_x)
            kind = (s + high) % 2
            y = x + kind - 2 * x * kind
            send_to(place(x, y, s // 2, high, high))

    loads[0].wait()

    @pl.when(my_inner == 0)
    def _():
        for s in range(seqs):
            ready(s)
            if s == 0:
                pl.semaphore_wait(barrier, devices - 1)
                tell(ends.at[my_high], other_kind)
            for turn_high, outer, turn_x in ((1, 1, 1), (1, 1, 0), (1, 0, 1), (1, 0, 0), (0, 0, 1), (0, 0, 0), (0, 1, 1), (0, 1, 0)):
                where = first_of(s, turn_high, outer, turn_x)
                if turn_high or turn_x:
                    send_to(where)
                else:
                    send_but_me(where)

    @pl.when(my_inner == 1)
    def _():
        for s in range(seqs):
            ready(s)
        pl.semaphore_wait(barrier, devices // 2 - 1)
        for s in range(seqs):
            for turn_x in (1, 0):
                send_to(first_of(s, 1, 1, turn_x))
        pl.semaphore_wait(ends.at[1], devices // 4)
        for s in range(seqs):
            to_end(s, 1)
        pl.semaphore_wait(ends.at[0], devices // 4)
        for s in range(seqs):
            to_end(s, 0)
        for s in range(seqs):
            send_to(first_of(s, 0, 1, 1))
            send_but_me(first_of(s, 0, 1, 0))

    held[me] = send[my_slot]

    for load in loads[1:4]:
        load.wait()
    for g in range(groups):
        rows = slice(g * width, (g + 1) * width)
        maps = jnp.dot(unpack_ref[...], given_ref[g], preferred_element_type=f32).astype(bf16)
        weights[rows, :] = jnp.dot(
            maps, outs_ref[rows, :], preferred_element_type=f32
        ).astype(bf16)
    for load in loads[4:]:
        load.wait()
    tile = twist_a.shape[2]
    row_ids = lax.broadcasted_iota(jnp.int32, (tile, positions), 0)
    for kind in range(2):
        is_sine = lax.rem(row_ids, 2) == 1
        if kind == 1:
            is_sine = is_sine & (row_ids != 1)
        for f in range(devices):
            cosine, sine = cos_ref[f : f + 1, :], sin_ref[f : f + 1, :]
            twist_a[kind, f] = jnp.where(is_sine, sine, cosine)
            twist_b[kind, f] = jnp.where(is_sine, -cosine, sine)
    several(send, held, devices - 1, send_sem, recv_sem).wait_recv()

    def spin(chunk, carry):
        rows = pl.ds(pl.multiple_of(chunk * tile, tile), tile)
        kind = jnp.where((chunk == 0) & (lax.rem(my_slot, 2) == 0), 1, 0)
        spun = fourier([held[d, rows, :].astype(f32) for d in range(devices)])
        for f in range(devices):
            real, imag = spun[min(f, devices - f)]
            turn_a, turn_b = twist_a[kind, f], twist_b[kind, f]
            if imag is None:
                first, second = real * turn_a, -(real * turn_b)
            elif 2 * f < devices:
                first, second = real * turn_a + imag * turn_b, imag * turn_a - real * turn_b
            else:
                first, second = real * turn_a - imag * turn_b, -(imag * turn_a + real * turn_b)
            stack[f, rows, :positions] = first.astype(bf16)
            stack[f, rows, positions:] = second.astype(bf16)
        return carry

    lax.fori_loop(0, items // tile, spin, 0)
    pairs = devices // 2
    for a in range(0, pairs, 2):
        both = jnp.concatenate(
            [stack[a], stack[a + pairs], stack[a + 1], stack[a + 1 + pairs]], axis=0
        )
        made = lax.dot_general(table_ref[...], both, rows_t, preferred_element_type=f32)
        big[pl.ds(a, positions, stride=pairs), :] = made[:, :width]
        big[pl.ds(a + 1, positions, stride=pairs), :] = made[:, width:]
    for e in range(devices):
        send_back[e] = big[e * items : (e + 1) * items, :].astype(bf16)

    def back_to(where, first):
        to_row, to_col, _ = where

        def go():
            slot_copy(
                send_back, to_row * cols + to_col, back, my_slot, send_back_sem,
                recv_back_sem.at[my_seq], (to_row, to_col),
            ).start()

        at = to_row * cols + to_col
        if first:
            pl.when(at != me)(go)
        else:
            pl.when((at != me) & (at >= 8))(go)

    for to_col in range(8):
        back_to((0, to_col, None), True)
    for level, step, core in ((0, 3, 1), (0, 3, 0), (0, 2, 1), (0, 2, 0), (1, 3, 1), (0, 1, 1), (1, 3, 0), (0, 1, 0), (1, 2, 1), (0, 0, 1), (1, 2, 0), (0, 0, 0), (1, 1, 1), (1, 1, 0), (1, 0, 1), (1, 0, 0), (2, 3, 1), (2, 3, 0), (2, 2, 1), (2, 2, 0), (3, 3, 1), (2, 1, 1), (3, 3, 0), (2, 1, 0), (3, 2, 1), (2, 0, 1), (3, 2, 0), (2, 0, 0), (3, 1, 1), (3, 1, 0), (3, 0, 1), (3, 0, 0)):
        x, y = other(my_x, step & 1), other(my_y, step >> 1)
        back_to(place(x, y, core, level % 2, level // 2), False)

    back[my_slot] = send_back[me]
    several(send, held, devices - 1, send_sem, recv_sem).wait_send()

    left = lax.broadcasted_iota(jnp.int32, (items, width), 1) < items

    def gather(s):
        @pl.when(my_seq == s)
        def _():
            several(send_back, back, members - 1, send_back_sem, recv_back_sem.at[s]).wait_recv()

        @pl.when(my_seq != s)
        def _():
            several(send_back, back, members, send_back_sem, recv_back_sem.at[s]).wait_recv()

        for g in range(groups):
            slot = s * members + g * 2
            first, second = back[slot].astype(f32), back[slot + 1].astype(f32)
            lanes = slice(g * width, (g + 1) * width)
            near[:items, lanes] = jnp.where(left, first, pltpu.roll(second, items, 1)).astype(bf16)
            near[items:, lanes] = jnp.where(left, pltpu.roll(first, items, 1), second).astype(bf16)

    def finish(s, carry):
        gather(s)
        product(near, weights, out_ref.at[s], devices)
        return carry

    lax.fori_loop(0, seqs - 1, finish, 0)
    gather(seqs - 1)
    several(send_back, back, devices - 1, send_back_sem, recv_back_sem.at[0]).wait_send()


CHUNK = 512


def product(near, weights, out_ref, devices, done=None):
    positions = near.shape[0]
    items, pairs = positions // 2, devices // 2
    for at in range(0, weights.shape[1], CHUNK):
        made = jnp.dot(
            near[...], weights[:, at : at + CHUNK], preferred_element_type=jnp.float32
        ).astype(jnp.bfloat16)
        for h in range(2):
            for m in range(items // pairs):
                base, had = m * devices + h * pairs, h * items + m * pairs
                out_ref[base : base + pairs, at : at + CHUNK] = made[had : had + pairs]
        if done is not None:
            done(at)


def last_kernel(devices, early, near, weights, out_hbm, late, early_sem, late_sem):
    seqs = early.shape[0] + 1
    early_copies = [
        pltpu.make_async_copy(early.at[s], out_hbm.at[s], early_sem.at[s]) for s in range(seqs - 1)
    ]
    for copy in early_copies:
        copy.start()
    late_copies = []

    def done(at):
        lanes = pl.ds(at, CHUNK)
        copy = pltpu.make_async_copy(
            late.at[:, lanes], out_hbm.at[seqs - 1, :, lanes], late_sem.at[at // CHUNK]
        )
        copy.start()
        late_copies.append(copy)

    product(near, weights, late, devices, done)
    for copy in early_copies + late_copies:
        copy.wait()


def fused_lanes(mix_input, group_maps, out_map, pack, unpack, devices, scale):
    bf16, f32 = jnp.bfloat16, jnp.float32
    seqs, positions, channels = mix_input.shape
    width = pack.shape[0]
    items = seqs * channels // devices
    length = devices * positions
    twist_cos, twist_sin = turn_tables(devices, positions, length)
    pos_cos, pos_sin = turn_tables(positions, positions, positions)
    table = np.concatenate([pos_cos, pos_sin], axis=1) * scale
    slots = (devices, items, positions)
    hbm = pl.BlockSpec(memory_space=pltpu.HBM)
    dma = pltpu.SemaphoreType.DMA
    vmem = pl.BlockSpec(memory_space=pltpu.VMEM)
    model = out_map.shape[1]
    given = (
        mix_input, jnp.asarray(pack.T, bf16), jnp.asarray(twist_cos, f32),
        jnp.asarray(twist_sin, f32), jnp.asarray(table, bf16), jnp.asarray(unpack, bf16), group_maps,
        out_map,
    )
    early, near, weights = pl.pallas_call(
        mixing_kernel,
        out_shape=[
            pltpu.VMEM((seqs - 1, positions, model), bf16), pltpu.VMEM((positions, channels), bf16),
            pltpu.VMEM(out_map.shape, bf16),
        ],
        in_specs=[hbm] * 8,
        out_specs=[vmem] * 3,
        scratch_shapes=[
            pltpu.VMEM(mix_input.shape, bf16), pltpu.VMEM(pack.shape, bf16),
            pltpu.VMEM(twist_cos.shape, f32), pltpu.VMEM(twist_sin.shape, f32),
            pltpu.VMEM(table.shape, bf16), pltpu.VMEM(unpack.shape, bf16),
            pltpu.VMEM(group_maps.shape, bf16), pltpu.VMEM(out_map.shape, bf16), dma((seqs + 7,)),
            pltpu.VMEM(slots, bf16), pltpu.VMEM(slots, bf16),
            pltpu.VMEM((devices, items, 2 * positions), bf16),
            pltpu.VMEM((devices * items, width), f32),
            pltpu.VMEM(slots, bf16), pltpu.VMEM(slots, bf16),
            dma, dma, dma, dma((seqs,)),
            pltpu.VMEM((2, devices, 16, positions), f32), pltpu.VMEM((2, devices, 16, positions), f32),
            pltpu.SemaphoreType.REGULAR((2,)),
        ],
        compiler_params=pltpu.CompilerParams(
            collective_id=0, has_side_effects=True, vmem_limit_bytes=32 << 20
        ),
    )(*(pltpu.with_memory_space_constraint(value, pltpu.HBM) for value in given))
    kept = [pltpu.with_memory_space_constraint(value, pltpu.VMEM) for value in (early, near, weights)]
    return pl.pallas_call(
        functools.partial(last_kernel, devices),
        out_shape=jax.ShapeDtypeStruct((seqs, positions, model), bf16),
        in_specs=[vmem] * 3,
        out_specs=hbm,
        scratch_shapes=[
            pltpu.VMEM((positions, model), bf16), dma((seqs - 1,)), dma((model // CHUNK,)),
        ],
        compiler_params=pltpu.CompilerParams(vmem_limit_bytes=16 << 20),
    )(*kept)


def exchanged_lanes(mix_input, pack, width, devices, me, scale):
    bf16, f32 = jnp.bfloat16, jnp.float32
    seqs, positions, channels = mix_input.shape
    groups = channels // width
    length = devices * positions
    items = seqs * channels // devices
    lanes = jnp.einsum(
        "spgj,jc->sgcp",
        mix_input.reshape(seqs, positions, groups, width),
        jnp.asarray(pack, bf16),
        preferred_element_type=f32,
    ).astype(bf16)
    sent = lanes.reshape(devices, items, positions)
    held = lax.all_to_all(sent, AXES, split_axis=0, concat_axis=0, tiled=True)

    dev_cos, dev_sin = turn_tables(devices, devices, devices)
    both = jnp.asarray(np.concatenate([dev_cos, -dev_sin], axis=1), bf16)
    spun = jnp.einsum("df,dnp->fnp", both, held, preferred_element_type=f32)
    real_in, imag_in = spun[:devices], spun[devices:]
    twist_cos, twist_sin = turn_tables(devices, positions, length)
    twist_cos = jnp.asarray(twist_cos, f32)[:, None, :]
    twist_sin = jnp.asarray(twist_sin, f32)[:, None, :]
    real_part = real_in * twist_cos + imag_in * twist_sin
    imag_part = imag_in * twist_cos - real_in * twist_sin
    lane_ids = (me * items + jnp.arange(items, dtype=jnp.int32)) % width
    is_sine = ((lane_ids % 2 == 1) & (lane_ids != 1))[None, :, None]
    first = jnp.where(is_sine, -imag_part, real_part).astype(bf16)
    second = jnp.where(is_sine, real_part, imag_part).astype(bf16)
    stacked = jnp.concatenate([first, second], axis=2)
    pos_cos, pos_sin = turn_tables(positions, positions, positions)
    pos_table = jnp.asarray(np.concatenate([pos_cos, pos_sin], axis=0) * scale, bf16)
    freqs = jnp.einsum("pm,fnp->mfn", pos_table, stacked, preferred_element_type=f32).astype(bf16)

    freqs = freqs.reshape(devices, positions, items)
    back = lax.all_to_all(freqs, AXES, split_axis=0, concat_axis=0, tiled=True)
    parts = width // items
    back = back.reshape(seqs, groups, parts, positions, items)
    return back.transpose(0, 3, 1, 2, 4).reshape(seqs * positions, groups, width)


def per_device(mix_input, group_maps, out_map):
    bf16, f32 = jnp.bfloat16, jnp.float32
    seqs, positions, channels = mix_input.shape
    groups, width, _ = group_maps.shape
    devices = lax.axis_size("row") * lax.axis_size("col")
    me = lax.axis_index("row") * lax.axis_size("col") + lax.axis_index("col")
    items = seqs * channels // devices
    pack, unpack = lane_tables(width)
    scale = 1.0 / math.sqrt(devices * positions * width)
    square = 2 * items == width and positions == width and items == 2 * devices
    if square and lax.axis_size("col") == 8 and seqs == 4:
        return fused_lanes(mix_input, group_maps, out_map, pack, unpack, devices, scale)
    back = exchanged_lanes(mix_input, pack, width, devices, me, scale)
    maps = jnp.einsum(
        "cl,glm->gcm", jnp.asarray(unpack, bf16), group_maps, preferred_element_type=f32
    ).astype(bf16)
    grouped = jnp.einsum("rgc,gcm->rgm", back, maps, preferred_element_type=f32).astype(bf16)
    mixed = jnp.dot(
        grouped.reshape(seqs * positions, channels), out_map, preferred_element_type=f32
    )
    return mixed.astype(bf16).reshape(seqs, positions, out_map.shape[1])


def solution(mesh):
    return jax.shard_map(
        per_device,
        mesh=mesh,
        in_specs=(P(None, AXES, None), P(), P()),
        out_specs=P(None, AXES, None),
        check_vma=False,
    )
```
